32 devices in a mesh: ep: 8 (over z, x), tp: 4 (over y, core).
Axes of the slice: x: 2, y: 2, z: 4, core: 2. Of those that a mesh axis runs over, the one named last changes fastest.
Arguments:
- hidden: bfloat16 [32, 2048], P('ep'), may hold values from -6 to 6
- attn_gain: float32 [2048], replicated, may hold values from 0.3 to 3
- query_weight: bfloat16 [2048, 2048], P('ep', 'tp'), may hold values from -0.125 to 0.125
- head_bias: float32 [16], replicated, may hold values from -10 to -4
- key_cache: bfloat16 [32, 4, 1024, 128], P('ep', 'tp'), may hold values from -6 to 6
- value_cache: bfloat16 [32, 4, 1024, 128], P('ep', 'tp'), may hold values from -7 to 7
- lengths: int32 [32], P('ep'), may hold values from 256 to 1024, as said below
- out_weight: bfloat16 [2048, 2048], P('tp', 'ep'), may hold values from -0.125 to 0.125
- moe_gain: float32 [2048], replicated, may hold values from 0.1 to 1.9
- route_group: int32 [32], P('ep'), may hold values from 0 to 1, as said below
- route_inner: int32 [32, 2], P('ep'), may hold values from 0 to 3, as said below
- route_weight: bfloat16 [32, 2], P('ep'), may hold values from 0.25 to 1
- gate_w: bfloat16 [8, 2048, 768], P('ep', None, 'tp'), may hold values from -0.125 to 0.125
- up_w: bfloat16 [8, 2048, 768], P('ep', None, 'tp'), may hold values from -0.125 to 0.125
- down_w: bfloat16 [8, 768, 2048], P('ep', 'tp'), may hold values from -0.21875 to 0.21875
Outputs:
- mixed: bfloat16 [32, 2048], P('ep', 'tp')
The draws below stay inside these ranges and needn't reach their ends.
Inputs may be any that keep to these rules, and one draw needn't show every extreme that they name: `lengths`: some sequence has length 1024 in every draw. Within the rows of one device (aligned blocks of 4 rows) no expert route_group * 4 + route_inner is named twice; one expert is named in every block. `route_inner`: the 2 entries of a row differ.
All inputs are finite; a program needn't handle non-finite values.
Results may differ from the reference program's by a relative error of at most 0.013.
Values may be sent and summed in bfloat16 or wider, within the bound.
No kernel may reach another device: no remote copies, remote signals or barrier semaphores. Data moves between devices by JAX's collectives and lax.ppermute only.
A program may use at most 64 MiB of HBM per device.

```python
import math
import jax
import jax.numpy as jnp
from jax import lax

D = 2048
HEADS = 16
KV_HEADS = 4
HEAD_SIZE = 128
FF_EXP = 768
TOPK = 2
SEQ_DEV = 4
CACHE = 1024
TOKENS = 32
EXPERTS = 8
GROUPS = 2
GROUP_SIZE = 4
N_EP = 8
N_TP = 4


def routing_tables(key):
    base = jax.random.fold_in(key, 7001)
    key_hot, key_perm, key_pairs, key_star = jax.random.split(base, 4)
    blocks = TOKENS // SEQ_DEV
    pairs_total = EXPERTS // TOPK
    pairs_group = GROUP_SIZE // TOPK
    hottest = jax.random.randint(key_hot, (), 0, EXPERTS)
    hot_group = hottest // GROUP_SIZE
    hot_inner = hottest % GROUP_SIZE
    perm_keys = jax.random.split(key_perm, blocks * GROUPS)
    perms = jax.vmap(lambda one_key: jax.random.permutation(one_key, GROUP_SIZE))(perm_keys)
    perms = perms.reshape(blocks, GROUPS, GROUP_SIZE)
    hot_perm = perms[:, hot_group, :]
    hot_place = jnp.argmax((hot_perm == hot_inner).astype(jnp.int32), axis=1)
    hot_pair = hot_group * pairs_group + hot_place // TOPK
    pair_keys = jax.random.split(key_pairs, blocks)
    order = jax.vmap(lambda one_key: jax.random.permutation(one_key, pairs_total))(pair_keys)
    hot_pos = jnp.argmax((order == hot_pair[:, None]).astype(jnp.int32), axis=1)
    starred = jax.random.randint(key_star, (blocks,), 0, SEQ_DEV)
    at_star = jnp.take_along_axis(order, starred[:, None], axis=1)[:, 0]
    places = jnp.arange(pairs_total)[None, :]
    order = jnp.where(places == starred[:, None], hot_pair[:, None], jnp.where(places == hot_pos[:, None], at_star[:, None], order))
    picked = order[:, :SEQ_DEV]
    groups = picked // pairs_group
    within = picked % pairs_group
    slot_index = within[:, :, None] * TOPK + jnp.arange(TOPK)[None, None, :]
    own_perm = perms[jnp.arange(blocks)[:, None], groups]
    inner = jnp.take_along_axis(own_perm, slot_index, axis=2)
    return (groups.reshape(TOKENS).astype(jnp.int32), inner.reshape(TOKENS, TOPK).astype(jnp.int32))


def draw_route_group(key, part):
    return routing_tables(key)[0]


def draw_route_inner(key, part):
    return routing_tables(key)[1]


def draw_lengths(key, part):
    base = jax.random.fold_in(key, 7101)
    key_len, key_top = jax.random.split(base, 2)
    spans = jax.random.randint(key_len, (TOKENS,), CACHE // 4, CACHE + 1)
    longest = jax.random.randint(key_top, (), 0, TOKENS)
    return jnp.where(jnp.arange(TOKENS) == longest, CACHE, spans).astype(jnp.int32)


def draw_head_bias(key, part):
    base = jax.random.fold_in(key, 7201)
    values = jax.random.uniform(base, (HEADS,), jnp.float32, -10.0, -4.0)
    return values


def draw_value_cache(key, part):
    base = jax.random.fold_in(key, 7301)
    key_common, key_noise = jax.random.split(base, 2)
    common = jax.random.normal(key_common, (TOKENS, KV_HEADS, 1, HEAD_SIZE), jnp.float32)
    noise = jax.random.normal(key_noise, (TOKENS, KV_HEADS, CACHE, HEAD_SIZE), jnp.float32)
    values = common + noise
    return jnp.clip(values, -7.0, 7.0).astype(jnp.bfloat16)


def levels(rng, dims, pieces, smallest, largest):
    level, own = 1.0, jax.random.fold_in(rng, 6)
    for position, parts in pieces:
        draws = jnp.exp(jax.random.uniform(jax.random.fold_in(own, position), (parts,), jnp.float32, smallest / len(pieces), largest / len(pieces)))
        level = level * jnp.repeat(draws, dims[position] // parts).reshape([-1 if axis == position else 1 for axis in range(len(dims))])
    return level


def centred(rng, dims, deviation, most, pieces=(), held_as=jnp.bfloat16):
    drawn = jax.random.normal(rng, dims, jnp.float32) * deviation
    if len(pieces) > 0:
        drawn = levels(rng, dims, pieces, -0.22, 0.18) * drawn
    return jnp.clip(drawn, min=-most, max=most).astype(held_as)


def setup_inputs(seed: int = 0) -> dict:
    streams_of = jax.random.split(jax.random.key(seed), 16)
    return {
        "hidden": centred(streams_of[0], (TOKENS, D), 1.0, 6.0, ((0, 8),)),
        "attn_gain": jnp.clip(jnp.exp(jax.random.uniform(streams_of[1], (D,), jnp.float32, math.log(0.3), math.log(3.0))), 0.3, 3.0),
        "query_weight": centred(streams_of[2], (D, HEADS * HEAD_SIZE), D ** -0.5, 0.125, ((0, 8), (1, 4))),
        "head_bias": draw_head_bias(jax.random.fold_in(streams_of[15], 71), 0),
        "key_cache": centred(streams_of[4], (TOKENS, KV_HEADS, CACHE, HEAD_SIZE), 1.0, 6.0, ((0, 8), (1, 4))),
        "value_cache": draw_value_cache(jax.random.fold_in(streams_of[15], 71), 0),
        "lengths": draw_lengths(jax.random.fold_in(streams_of[15], 71), 0),
        "out_weight": centred(streams_of[7], (HEADS * HEAD_SIZE, D), (HEADS * HEAD_SIZE) ** -0.5, 0.125, ((0, 4), (1, 8))),
        "moe_gain": jnp.clip(1.0 + 0.18 * jax.random.normal(streams_of[8], (D,), jnp.float32), 0.1, 1.9),
        "route_group": draw_route_group(jax.random.fold_in(streams_of[15], 71), 0),
        "route_inner": draw_route_inner(jax.random.fold_in(streams_of[15], 71), 0),
        "route_weight": jnp.clip(0.25 + 0.75 * jax.random.uniform(streams_of[11], (TOKENS, TOPK), jnp.float32) ** levels(streams_of[11], (TOKENS, TOPK), ((0, 8),), -0.2, 0.2), 0.25, 1.0).astype(jnp.bfloat16),
        "gate_w": centred(streams_of[12], (EXPERTS, D, FF_EXP), D ** -0.5, 0.125, ((0, 8), (2, 4))),
        "up_w": centred(streams_of[13], (EXPERTS, D, FF_EXP), D ** -0.5, 0.125, ((0, 8), (2, 4))),
        "down_w": centred(streams_of[14], (EXPERTS, FF_EXP, D), FF_EXP ** -0.5, 0.21875, ((0, 8), (1, 4))),
    }


rms_epsilon = 1e-06

def rms_scale(values, gain):
    wide = values.astype(jnp.float32)
    scaled = wide * lax.rsqrt(lax.optimization_barrier(jnp.mean(wide * wide, axis=-1, keepdims=True)) + rms_epsilon)
    return (scaled * gain).astype(jnp.bfloat16)

def attend(queries, key_cache, value_cache, lengths, head_bias):
    group_heads = HEADS // KV_HEADS
    bias_grid = head_bias.reshape(KV_HEADS, group_heads)

    def one_sequence(args):
        query_row, keys, values, length = args
        grouped = query_row.reshape(KV_HEADS, group_heads, HEAD_SIZE).astype(jnp.float32)
        scores = jnp.einsum('kgd,kpd->kgp', grouped, keys.astype(jnp.float32)) * HEAD_SIZE ** (-0.5)
        scores = scores + bias_grid[:, :, None]
        visible = jnp.arange(CACHE, dtype=jnp.int32) < length
        log_keep = jnp.where(visible[None, None, :], jax.nn.log_sigmoid(-scores), 0.0)
        later_sum = lax.cumsum(log_keep, axis=2, reverse=True) - log_keep
        weight = jnp.where(visible[None, None, :], jnp.exp(jax.nn.log_sigmoid(scores) + later_sum), 0.0)
        weight = weight.astype(jnp.bfloat16)
        result = jnp.einsum('kgp,kpd->kgd', weight.astype(jnp.float32), values.astype(jnp.float32))
        return result.astype(jnp.bfloat16).reshape(HEADS, HEAD_SIZE)
    return lax.map(one_sequence, (queries, key_cache, value_cache, lengths))

def reference(hidden, attn_gain, query_weight, head_bias, key_cache, value_cache, lengths, out_weight, moe_gain, route_group, route_inner, route_weight, gate_w, up_w, down_w):
    normed = rms_scale(hidden, attn_gain)
    queries = jnp.dot(normed, query_weight, preferred_element_type=jnp.float32).astype(jnp.bfloat16)
    queries = queries.reshape(TOKENS, HEADS, HEAD_SIZE)
    heads_out = attend(queries, key_cache, value_cache, lengths, head_bias).reshape(TOKENS, HEADS * HEAD_SIZE)
    head_width = HEADS * HEAD_SIZE // N_TP
    attended = jnp.zeros((TOKENS, D), jnp.float32)
    for group in range(N_TP):
        partial_value = jnp.dot(heads_out[:, group * head_width:(group + 1) * head_width], out_weight[group * head_width:(group + 1) * head_width], preferred_element_type=jnp.float32)
        attended = attended + lax.optimization_barrier(partial_value.astype(jnp.bfloat16)).astype(jnp.float32)
    residual = (hidden.astype(jnp.float32) + attended).astype(jnp.bfloat16)
    normed_two = rms_scale(residual, moe_gain)
    assigned = TOKENS * TOPK
    chosen = (route_group[:, None] * GROUP_SIZE + route_inner).reshape(assigned).astype(jnp.int32)
    padded_rows = jnp.concatenate([normed_two, jnp.zeros((1, D), jnp.bfloat16)], axis=0)
    weights_flat = jnp.concatenate([route_weight.reshape(assigned).astype(jnp.float32), jnp.zeros((1,), jnp.float32)], axis=0)
    ff_width = FF_EXP // N_TP

    def one_expert(expert):
        slots = jnp.nonzero(chosen == expert, size=N_EP, fill_value=assigned)[0].astype(jnp.int32)
        rows = padded_rows[slots // TOPK]
        gate_all = gate_w[expert]
        up_all = up_w[expert]
        down_all = down_w[expert]
        total = jnp.zeros((N_EP, D), jnp.float32)
        for group in range(N_TP):
            gated = jnp.dot(rows, gate_all[:, group * ff_width:(group + 1) * ff_width], preferred_element_type=jnp.float32)
            upped = jnp.dot(rows, up_all[:, group * ff_width:(group + 1) * ff_width], preferred_element_type=jnp.float32)
            activated = (jax.nn.silu(gated) * upped).astype(jnp.bfloat16)
            down_part = jnp.dot(activated, down_all[group * ff_width:(group + 1) * ff_width], preferred_element_type=jnp.float32)
            total = total + lax.optimization_barrier(down_part.astype(jnp.bfloat16)).astype(jnp.float32)
        return (slots, total.astype(jnp.bfloat16))
    slots, outputs = lax.map(one_expert, jnp.arange(EXPERTS, dtype=jnp.int32))
    contrib = weights_flat[slots][:, :, None] * outputs.astype(jnp.float32)
    collected = jnp.zeros((assigned + 1, D), jnp.float32).at[slots.reshape(-1)].add(contrib.reshape(-1, D))
    routed = lax.optimization_barrier(jnp.sum(collected[:assigned].reshape(TOKENS, TOPK, D), axis=1))
    return (residual.astype(jnp.float32) + routed).astype(jnp.bfloat16)
```

```python
import jax
import jax.numpy as jnp
from jax import lax
from jax.sharding import PartitionSpec as P

rms_epsilon = 1e-06


def body(
    hidden,
    attn_gain,
    query_weight,
    head_bias,
    key_cache,
    value_cache,
    lengths,
    out_weight,
    moe_gain,
    route_group,
    route_inner,
    route_weight,
    gate_w,
    up_w,
    down_w,
):
    f32, bf16 = jnp.float32, jnp.bfloat16
    n_tp = lax.axis_size("tp")
    n_ep = lax.axis_size("ep")
    tokens, d_model = hidden.shape
    rows = query_weight.shape[0]
    per_device = gate_w.shape[0]
    experts = per_device * n_ep
    group_count = max(2, experts // 32)
    group_size = experts // group_count
    top_k = route_inner.shape[1]
    chosen = route_group[:, None] * group_size + route_inner

    blocks = hidden.reshape(tokens, n_ep, rows).transpose(1, 0, 2).reshape(n_ep, tokens * rows)
    ids = jnp.broadcast_to(chosen.astype(bf16).reshape(1, tokens * top_k), (n_ep, tokens * top_k))
    ids = jnp.pad(ids, ((0, 0), (0, 128 - tokens * top_k)))
    packed = jnp.concatenate([blocks, ids], axis=1)
    packed = lax.all_to_all(packed, "ep", split_axis=0, concat_axis=0, tiled=True)
    all_tokens = n_ep * tokens
    features = packed[:, : tokens * rows].reshape(all_tokens, rows)
    all_chosen = packed[:, tokens * rows : tokens * (rows + top_k)].reshape(all_tokens, top_k)
    all_chosen = all_chosen.astype(jnp.int32)

    ep_index = lax.axis_index("ep")
    gain_block = lax.dynamic_slice_in_dim(attn_gain, ep_index * rows, rows, 0)
    scaled = (features.astype(f32) * gain_block).astype(bf16)
    parts = jnp.dot(scaled, query_weight, preferred_element_type=f32)
    width = parts.shape[1]

    parts = lax.all_to_all(
        parts.reshape(n_ep, tokens * width), "ep", split_axis=0, concat_axis=0, tiled=True
    )
    wide = hidden.astype(f32)
    row_scale = lax.rsqrt(jnp.mean(wide * wide, axis=-1, keepdims=True) + rms_epsilon)
    queries = parts.sum(axis=0).reshape(tokens, width) * row_scale
    queries = queries.astype(bf16)

    head_size = key_cache.shape[3]
    local_kv = key_cache.shape[1]
    cache_len = key_cache.shape[2]
    local_heads = width // head_size
    group_heads = local_heads // local_kv
    queries = queries.reshape(tokens, local_kv, group_heads, head_size)
    own_bias = lax.dynamic_slice_in_dim(
        head_bias, lax.axis_index("tp") * local_heads, local_heads, 0
    )
    own_bias = own_bias.reshape(local_kv, group_heads)
    scores = jnp.einsum(
        "tkgd,tkpd->tkgp", queries, key_cache, preferred_element_type=f32
    ) * head_size ** (-0.5)
    scores = scores + own_bias[None, :, :, None]
    position = jnp.arange(cache_len, dtype=jnp.int32)
    visible = position[None, None, None, :] < lengths[:, None, None, None]
    soft = jnp.log1p(jnp.exp(-jnp.abs(scores)))
    log_keep = jnp.where(visible, -jnp.maximum(scores, 0.0) - soft, 0.0)
    n_chunk = cache_len // 128
    chunked = log_keep.reshape(tokens, local_kv, group_heads, n_chunk, 128)
    lower = (jnp.arange(128)[:, None] > jnp.arange(128)[None, :]).astype(f32)
    inner = jnp.einsum("tkgcp,pq->tkgcq", chunked, lower, precision=lax.Precision.HIGHEST)
    totals = chunked.sum(axis=-1)
    later_chunks = jnp.arange(n_chunk)[:, None] > jnp.arange(n_chunk)[None, :]
    outer = jnp.where(later_chunks, totals[..., :, None], 0.0).sum(axis=-2)
    later_sum = (inner + outer[..., None]).reshape(scores.shape)
    weight = jnp.where(visible, jnp.exp(jnp.minimum(scores, 0.0) - soft + later_sum), 0.0)
    heads_out = jnp.einsum(
        "tkgp,tkpd->tkgd", weight.astype(bf16), value_cache, preferred_element_type=f32
    )
    heads_out = heads_out.astype(bf16).reshape(1, tokens * width)

    gathered = lax.all_to_all(
        jnp.broadcast_to(heads_out, (n_ep, tokens * width)), "ep", split_axis=0, concat_axis=0, tiled=True
    ).reshape(all_tokens, width)
    partial = jnp.dot(gathered, out_weight, preferred_element_type=f32)
    columns = out_weight.shape[1]
    partial = (partial + features.astype(f32) * (1.0 / n_tp)).astype(bf16)

    by_block = all_chosen.reshape(n_ep, tokens, top_k)
    hits = by_block[None] == jnp.arange(experts, dtype=jnp.int32)[:, None, None, None]
    hits = jnp.any(hits, axis=3).astype(bf16)
    routed = jnp.einsum(
        "ebt,btc->ebc", hits, partial.reshape(n_ep, tokens, columns), preferred_element_type=f32
    ).astype(bf16)
    routed = routed.reshape(n_ep, per_device * n_ep * columns)
    message = jnp.concatenate([routed, partial.reshape(n_ep, tokens * columns)], axis=1)
    length = message.shape[1]
    message = jnp.broadcast_to(message[:, None], (n_ep, n_tp, length)).reshape(n_ep * n_tp, length)
    received = lax.all_to_all(message, ("ep", "tp"), split_axis=0, concat_axis=0, tiled=True)
    received = received.reshape(n_ep, n_tp, per_device * n_ep + tokens, columns)
    summed = received.astype(f32).sum(axis=1)
    residual = summed.transpose(1, 0, 2).reshape(per_device * n_ep + tokens, d_model)
    arrived = residual[: per_device * n_ep]
    arrived = arrived * lax.rsqrt(jnp.mean(arrived * arrived, axis=-1, keepdims=True) + rms_epsilon)
    arrived = (arrived * moe_gain).astype(bf16).reshape(per_device, n_ep, d_model)
    gated_in = jnp.einsum("esd,edf->esf", arrived, gate_w, preferred_element_type=f32)
    up_proj = jnp.einsum("esd,edf->esf", arrived, up_w, preferred_element_type=f32)
    activated = (jax.nn.silu(gated_in) * up_proj).astype(bf16)
    down_out = jnp.einsum("esf,efd->sed", activated, down_w, preferred_element_type=f32).astype(bf16)

    part_width = d_model // n_tp
    down_out = down_out.reshape(n_ep, per_device, n_tp, part_width).transpose(0, 2, 1, 3)
    returned = lax.all_to_all(
        down_out.reshape(n_ep * n_tp, per_device * part_width), ("ep", "tp"), split_axis=0, concat_axis=0, tiled=True
    )
    returned = returned.reshape(n_ep, n_tp, per_device, part_width).astype(f32).sum(axis=1)
    returned = returned.reshape(experts, part_width)
    matches = chosen[:, :, None] == jnp.arange(experts, dtype=jnp.int32)[None, None, :]
    mixing = jnp.sum(jnp.where(matches, route_weight[:, :, None].astype(f32), 0.0), axis=1)
    mixed = jnp.sum(mixing[:, :, None] * returned[None], axis=1)
    own_residual = lax.dynamic_slice_in_dim(
        residual[per_device * n_ep :], lax.axis_index("tp") * part_width, part_width, 1
    )
    return (own_residual + mixed).astype(bf16)


def solution(mesh):
    placed = (
        P("ep", None),
        P(),
        P("ep", "tp"),
        P(),
        P("ep", "tp", None, None),
        P("ep", "tp", None, None),
        P("ep"),
        P("tp", "ep"),
        P(),
        P("ep"),
        P("ep", None),
        P("ep", None),
        P("ep", None, "tp"),
        P("ep", None, "tp"),
        P("ep", "tp", None),
    )
    return jax.shard_map(body, mesh=mesh, in_specs=placed, out_specs=P("ep", "tp"), check_vma=False)
```

```python
import jax
import jax.numpy as jnp
from jax import lax
from jax.experimental import pallas as pl
from jax.experimental.pallas import tpu as pltpu
from jax.sharding import PartitionSpec as P

rms_epsilon = 1e-06
f32, bf16, i32 = jnp.float32, jnp.bfloat16, jnp.int32
in_vmem = pl.BlockSpec(memory_space=pltpu.VMEM)
in_smem = pl.BlockSpec(memory_space=pltpu.SMEM)


def send_kernel(hidden_ref, group_ref, inner_ref, out_ref, *, group_size):
    n_ep, height, rows = out_ref.shape
    tokens, top_k = inner_ref.shape
    lane = lax.broadcasted_iota(i32, (tokens, rows), 1)
    ids = jnp.zeros((tokens, rows), f32)
    for t in range(tokens):
        for k in range(top_k):
            value = (group_ref[t] * group_size + inner_ref[t, k]).astype(f32)
            ids = jnp.where(lane == t * top_k + k, value, ids)
    for e in range(n_ep):
        part = hidden_ref[:, e * rows : (e + 1) * rows].astype(f32)
        out_ref[e] = jnp.concatenate([part, ids], axis=0).astype(bf16)


def query_kernel(features_ref, gain_ref, weight_ref, out_ref, *, tokens):
    n_ep, height, rows = features_ref.shape
    heads = out_ref.shape[1] // tokens
    size = out_ref.shape[2]
    gain = gain_ref[pl.ds(lax.axis_index("ep"), 1), :]
    flat = features_ref[...].astype(f32).reshape(n_ep * height, rows)
    parts = jnp.dot((flat * gain).astype(bf16), weight_ref[...], preferred_element_type=f32)
    parts = parts.reshape(n_ep, height, heads * size)
    for h in range(heads):
        out_ref[:, h * tokens : (h + 1) * tokens, :] = parts[:, :tokens, h * size : (h + 1) * size]


def attend_kernel(
    parts_ref, hidden_ref, key_ref, value_ref, lengths_ref, bias_ref, out_ref
):
    tokens, _, cache, size = key_ref.shape
    n_ep, rows, _ = parts_ref.shape
    heads = rows // tokens
    chunk = 128
    wide = hidden_ref[...].astype(f32)
    scale = lax.rsqrt(jnp.mean(wide * wide, axis=-1, keepdims=True) + rms_epsilon)
    queries = jnp.sum(parts_ref[...], axis=0) * jnp.concatenate([scale] * heads, axis=0)
    queries = queries.astype(bf16)
    row = lax.broadcasted_iota(i32, (rows, 1), 0)
    token_of, head_of = row % tokens, row // tokens
    bias = jnp.zeros((rows, 1), f32)
    first = lax.axis_index("tp") * heads
    for h in range(heads):
        bias = jnp.where(head_of == h, bias_ref[first + h], bias)
    length = jnp.zeros((rows, 1), i32)
    for t in range(tokens):
        length = jnp.where(token_of == t, lengths_ref[t], length)
    scores = jnp.zeros((rows, cache), f32)
    for t in range(tokens):
        found = lax.dot_general(
            queries, key_ref[t, 0], (((1,), (1,)), ((), ())), preferred_element_type=f32
        )
        scores = jnp.where(token_of == t, found, scores)
    scores = scores * size ** (-0.5) + bias
    visible = lax.broadcasted_iota(i32, (rows, cache), 1) < length
    soft = jnp.log1p(jnp.exp(-jnp.abs(scores)))
    log_keep = jnp.where(visible, -jnp.maximum(scores, 0.0) - soft, 0.0)
    log_take = jnp.minimum(scores, 0.0) - soft
    count = cache // chunk
    stacked = jnp.concatenate([log_keep[:, c * chunk : (c + 1) * chunk] for c in range(count)], axis=0)
    later = (
        lax.broadcasted_iota(i32, (chunk, chunk), 0) > lax.broadcasted_iota(i32, (chunk, chunk), 1)
    ).astype(f32)
    inner = jnp.dot(stacked, later, preferred_element_type=f32, precision=lax.Precision.HIGHEST)
    totals = jnp.sum(stacked, axis=1, keepdims=True)
    running = jnp.zeros((rows, 1), f32)
    pieces = [None] * count
    for c in reversed(range(count)):
        pieces[c] = inner[c * rows : (c + 1) * rows] + running
        running = running + totals[c * rows : (c + 1) * rows]
    later_sum = jnp.concatenate(pieces, axis=1)
    weight = jnp.where(visible, jnp.exp(log_take + later_sum), 0.0).astype(bf16)
    result = jnp.zeros((rows, size), f32)
    for t in range(tokens):
        found = jnp.dot(weight, value_ref[t, 0], preferred_element_type=f32)
        result = jnp.where(token_of == t, found, result)
    result = result.astype(bf16)
    for e in range(n_ep):
        out_ref[e] = result


def project_kernel(heads_ref, weight_ref, features_ref, pick_ref, out_ref, *, tokens, n_tp):
    n_ep, rows, size = heads_ref.shape
    heads = rows // tokens
    height, columns = features_ref.shape[1:]
    flat = heads_ref[...].reshape(n_ep * rows, size)
    total = features_ref[...].astype(f32) * (1.0 / n_tp)
    total = total[:, :tokens, :]
    for h in range(heads):
        found = jnp.dot(
            flat, weight_ref[h * size : (h + 1) * size, :], preferred_element_type=f32
        ).reshape(n_ep, rows, columns)
        total = total + found[:, h * tokens : (h + 1) * tokens, :]
    total = jnp.concatenate([total, jnp.zeros((n_ep, height - tokens, columns), f32)], axis=1)
    total = total.reshape(n_ep * height, columns).astype(bf16)
    message = jnp.dot(pick_ref[...], total, preferred_element_type=f32).astype(bf16)
    message = message.reshape(n_ep, out_ref.shape[2], columns)
    for g in range(n_tp):
        out_ref[:, g] = message


def expert_kernel(parts_ref, gain_ref, gate_ref, up_ref, down_ref, out_ref, own_ref, *, tokens):
    n_ep, n_tp, height, columns = parts_ref.shape
    size = out_ref.shape[2]
    pieces = []
    for e in range(n_ep):
        piece = parts_ref[e, 0].astype(f32)
        for g in range(1, n_tp):
            piece = piece + parts_ref[e, g].astype(f32)
        pieces.append(piece)
    residual = jnp.concatenate(pieces, axis=1)
    own_ref[...] = residual[n_ep:, :]
    arrived = residual[:n_ep, :]
    arrived = arrived * lax.rsqrt(jnp.mean(arrived * arrived, axis=-1, keepdims=True) + rms_epsilon)
    arrived = (arrived * gain_ref[...]).astype(bf16)
    gated = jnp.dot(arrived, gate_ref[0], preferred_element_type=f32)
    up = jnp.dot(arrived, up_ref[0], preferred_element_type=f32)
    active = (gated / (1.0 + jnp.exp(-gated)) * up).astype(bf16)
    down = jnp.dot(active, down_ref[0], preferred_element_type=f32)
    for j in range(out_ref.shape[1]):
        out_ref[:, j, :] = down[:, j * size : (j + 1) * size]


def fast_body(
    hidden,
    attn_gain,
    query_weight,
    head_bias,
    key_cache,
    value_cache,
    lengths,
    out_weight,
    moe_gain,
    route_group,
    route_inner,
    route_weight,
    gate_w,
    up_w,
    down_w,
):
    n_tp = lax.axis_size("tp")
    n_ep = lax.axis_size("ep")
    tokens, d_model = hidden.shape
    rows, width = query_weight.shape
    columns = out_weight.shape[1]
    size = key_cache.shape[3]
    heads = width // size
    experts = n_ep
    group_size = experts // max(2, experts // 32)
    top_k = route_inner.shape[1]
    height = 2 * tokens
    part_width = d_model // n_tp
    call = pl.pallas_call

    packed = call(
        lambda *refs: send_kernel(*refs, group_size=group_size),
        name="send",
        out_shape=jax.ShapeDtypeStruct((n_ep, height, rows), bf16),
        in_specs=[in_vmem, in_smem, in_smem],
        out_specs=in_vmem,
    )(hidden, route_group, route_inner)
    packed = lax.all_to_all(packed, "ep", split_axis=0, concat_axis=0, tiled=True)

    parts = call(
        lambda *refs: query_kernel(*refs, tokens=tokens),
        name="query",
        out_shape=jax.ShapeDtypeStruct((n_ep, heads * tokens, size), f32),
        in_specs=[in_vmem] * 3,
        out_specs=in_vmem,
    )(packed, attn_gain.reshape(n_ep, rows), query_weight)
    parts = lax.all_to_all(parts, "ep", split_axis=0, concat_axis=0, tiled=True)

    heads_out = call(
        attend_kernel,
        name="attend",
        out_shape=jax.ShapeDtypeStruct((n_ep, heads * tokens, size), bf16),
        in_specs=[in_vmem] * 4 + [in_smem] * 2,
        out_specs=in_vmem,
    )(parts, hidden, key_cache, value_cache, lengths, head_bias)
    heads_out = lax.all_to_all(heads_out, "ep", split_axis=0, concat_axis=0, tiled=True)

    named = packed[:, tokens, : tokens * top_k].reshape(n_ep, tokens, top_k).astype(i32)
    named = jnp.pad(named, ((0, 0), (0, height - tokens), (0, 0)), constant_values=-1)
    named = named.reshape(1, 1, n_ep, height, top_k)
    message_rows = -(-(n_ep + tokens) // 16) * 16
    shape = (n_ep, message_rows, n_ep, height)
    expert = lax.broadcasted_iota(i32, shape, 0)
    slot = lax.broadcasted_iota(i32, shape, 1)
    block = lax.broadcasted_iota(i32, shape, 2)
    place = lax.broadcasted_iota(i32, shape, 3)
    hit = jnp.any(named == expert[..., None], axis=-1)
    pick = ((slot == block) & hit) | ((block == expert) & (slot == n_ep + place) & (place < tokens))
    pick = pick.astype(bf16).reshape(n_ep * message_rows, n_ep * height)

    message = call(
        lambda *refs: project_kernel(*refs, tokens=tokens, n_tp=n_tp),
        name="project",
        out_shape=jax.ShapeDtypeStruct((n_ep, n_tp, message_rows, columns), bf16),
        in_specs=[in_vmem] * 4,
        out_specs=in_vmem,
    )(heads_out, out_weight, packed, pick)
    message = message.reshape(n_ep * n_tp, message_rows, columns)
    message = lax.all_to_all(message, ("ep", "tp"), split_axis=0, concat_axis=0, tiled=True)

    down_out, own = call(
        lambda *refs: expert_kernel(*refs, tokens=tokens),
        name="expert",
        out_shape=(
            jax.ShapeDtypeStruct((n_ep, d_model // size, size), f32),
            jax.ShapeDtypeStruct((message_rows - n_ep, d_model), f32),
        ),
        in_specs=[in_vmem] * 5,
        out_specs=(in_vmem, in_vmem),
    )(
        message.reshape(n_ep, n_tp, message_rows, columns),
        moe_gain.reshape(1, d_model),
        gate_w,
        up_w,
        down_w,
    )
    lanes = part_width // size
    returned = lax.all_to_all(
        down_out.reshape(n_ep * n_tp, lanes, size), ("ep", "tp"), split_axis=0, concat_axis=0, tiled=True
    )
    returned = returned.reshape(n_ep, n_tp, lanes, size).sum(axis=1)
    chosen = route_group[:, None] * group_size + route_inner
    matches = chosen[:, :, None] == jnp.arange(experts, dtype=i32)[None, None, :]
    mixing = jnp.sum(jnp.where(matches, route_weight[:, :, None].astype(f32), 0.0), axis=1)
    mixed = jnp.sum(mixing[:, :, None, None] * returned[None], axis=1).reshape(tokens, part_width)
    own = lax.dynamic_slice_in_dim(own[:tokens], lax.axis_index("tp") * part_width, part_width, 1)
    return (own + mixed).astype(bf16)


def body(*args):
    hidden, query_weight, key_cache = args[0], args[2], args[4]
    out_weight, gate_w = args[7], args[12]
    aligned = all(
        extent % 128 == 0
        for extent in (query_weight.shape[0], query_weight.shape[1], out_weight.shape[1])
    )
    single = gate_w.shape[0] == 1 and key_cache.shape[1] == 1
    shapes = hidden.shape[0] == 4 and key_cache.shape[3] == 128 and key_cache.shape[2] % 128 == 0
    return fast_body(*args) if aligned and single and shapes else plain_body(*args)


def plain_body(
    hidden,
    attn_gain,
    query_weight,
    head_bias,
    key_cache,
    value_cache,
    lengths,
    out_weight,
    moe_gain,
    route_group,
    route_inner,
    route_weight,
    gate_w,
    up_w,
    down_w,
):
    f32, bf16 = jnp.float32, jnp.bfloat16
    n_tp = lax.axis_size("tp")
    n_ep = lax.axis_size("ep")
    tokens, d_model = hidden.shape
    rows = query_weight.shape[0]
    per_device = gate_w.shape[0]
    experts = per_device * n_ep
    group_count = max(2, experts // 32)
    group_size = experts // group_count
    top_k = route_inner.shape[1]
    chosen = route_group[:, None] * group_size + route_inner

    blocks = hidden.reshape(tokens, n_ep, rows).transpose(1, 0, 2).reshape(n_ep, tokens * rows)
    ids = jnp.broadcast_to(chosen.astype(bf16).reshape(1, tokens * top_k), (n_ep, tokens * top_k))
    ids = jnp.pad(ids, ((0, 0), (0, 128 - tokens * top_k)))
    packed = jnp.concatenate([blocks, ids], axis=1)
    packed = lax.all_to_all(packed, "ep", split_axis=0, concat_axis=0, tiled=True)
    all_tokens = n_ep * tokens
    features = packed[:, : tokens * rows].reshape(all_tokens, rows)
    all_chosen = packed[:, tokens * rows : tokens * (rows + top_k)].reshape(all_tokens, top_k)
    all_chosen = all_chosen.astype(jnp.int32)

    ep_index = lax.axis_index("ep")
    gain_block = lax.dynamic_slice_in_dim(attn_gain, ep_index * rows, rows, 0)
    scaled = (features.astype(f32) * gain_block).astype(bf16)
    parts = jnp.dot(scaled, query_weight, preferred_element_type=f32)
    width = parts.shape[1]

    parts = lax.all_to_all(
        parts.reshape(n_ep, tokens * width), "ep", split_axis=0, concat_axis=0, tiled=True
    )
    wide = hidden.astype(f32)
    row_scale = lax.rsqrt(jnp.mean(wide * wide, axis=-1, keepdims=True) + rms_epsilon)
    queries = parts.sum(axis=0).reshape(tokens, width) * row_scale
    queries = queries.astype(bf16)

    head_size = key_cache.shape[3]
    local_kv = key_cache.shape[1]
    cache_len = key_cache.shape[2]
    local_heads = width // head_size
    group_heads = local_heads // local_kv
    queries = queries.reshape(tokens, local_kv, group_heads, head_size)
    own_bias = lax.dynamic_slice_in_dim(
        head_bias, lax.axis_index("tp") * local_heads, local_heads, 0
    )
    own_bias = own_bias.reshape(local_kv, group_heads)
    scores = jnp.einsum(
        "tkgd,tkpd->tkgp", queries, key_cache, preferred_element_type=f32
    ) * head_size ** (-0.5)
    scores = scores + own_bias[None, :, :, None]
    position = jnp.arange(cache_len, dtype=jnp.int32)
    visible = position[None, None, None, :] < lengths[:, None, None, None]
    soft = jnp.log1p(jnp.exp(-jnp.abs(scores)))
    log_keep = jnp.where(visible, -jnp.maximum(scores, 0.0) - soft, 0.0)
    n_chunk = cache_len // 128
    chunked = log_keep.reshape(tokens, local_kv, group_heads, n_chunk, 128)
    lower = (jnp.arange(128)[:, None] > jnp.arange(128)[None, :]).astype(f32)
    inner = jnp.einsum("tkgcp,pq->tkgcq", chunked, lower, precision=lax.Precision.HIGHEST)
    totals = chunked.sum(axis=-1)
    later_chunks = jnp.arange(n_chunk)[:, None] > jnp.arange(n_chunk)[None, :]
    outer = jnp.where(later_chunks, totals[..., :, None], 0.0).sum(axis=-2)
    later_sum = (inner + outer[..., None]).reshape(scores.shape)
    weight = jnp.where(visible, jnp.exp(jnp.minimum(scores, 0.0) - soft + later_sum), 0.0)
    heads_out = jnp.einsum(
        "tkgp,tkpd->tkgd", weight.astype(bf16), value_cache, preferred_element_type=f32
    )
    heads_out = heads_out.astype(bf16).reshape(1, tokens * width)

    gathered = lax.all_to_all(
        jnp.broadcast_to(heads_out, (n_ep, tokens * width)), "ep", split_axis=0, concat_axis=0, tiled=True
    ).reshape(all_tokens, width)
    partial = jnp.dot(gathered, out_weight, preferred_element_type=f32)
    columns = out_weight.shape[1]
    partial = (partial + features.astype(f32) * (1.0 / n_tp)).astype(bf16)

    by_block = all_chosen.reshape(n_ep, tokens, top_k)
    hits = by_block[None] == jnp.arange(experts, dtype=jnp.int32)[:, None, None, None]
    hits = jnp.any(hits, axis=3).astype(bf16)
    routed = jnp.einsum(
        "ebt,btc->ebc", hits, partial.reshape(n_ep, tokens, columns), preferred_element_type=f32
    ).astype(bf16)
    routed = routed.reshape(n_ep, per_device * n_ep * columns)
    message = jnp.concatenate([routed, partial.reshape(n_ep, tokens * columns)], axis=1)
    length = message.shape[1]
    message = jnp.broadcast_to(message[:, None], (n_ep, n_tp, length)).reshape(n_ep * n_tp, length)
    received = lax.all_to_all(message, ("ep", "tp"), split_axis=0, concat_axis=0, tiled=True)
    received = received.reshape(n_ep, n_tp, per_device * n_ep + tokens, columns)
    summed = received.astype(f32).sum(axis=1)
    residual = summed.transpose(1, 0, 2).reshape(per_device * n_ep + tokens, d_model)
    arrived = residual[: per_device * n_ep]
    arrived = arrived * lax.rsqrt(jnp.mean(arrived * arrived, axis=-1, keepdims=True) + rms_epsilon)
    arrived = (arrived * moe_gain).astype(bf16).reshape(per_device, n_ep, d_model)
    gated_in = jnp.einsum("esd,edf->esf", arrived, gate_w, preferred_element_type=f32)
    up_proj = jnp.einsum("esd,edf->esf", arrived, up_w, preferred_element_type=f32)
    activated = (jax.nn.silu(gated_in) * up_proj).astype(bf16)
    down_out = jnp.einsum("esf,efd->sed", activated, down_w, preferred_element_type=f32).astype(bf16)

    part_width = d_model // n_tp
    down_out = down_out.reshape(n_ep, per_device, n_tp, part_width).transpose(0, 2, 1, 3)
    returned = lax.all_to_all(
        down_out.reshape(n_ep * n_tp, per_device * part_width), ("ep", "tp"), split_axis=0, concat_axis=0, tiled=True
    )
    returned = returned.reshape(n_ep, n_tp, per_device, part_width).astype(f32).sum(axis=1)
    returned = returned.reshape(experts, part_width)
    matches = chosen[:, :, None] == jnp.arange(experts, dtype=jnp.int32)[None, None, :]
    mixing = jnp.sum(jnp.where(matches, route_weight[:, :, None].astype(f32), 0.0), axis=1)
    mixed = jnp.sum(mixing[:, :, None] * returned[None], axis=1)
    own_residual = lax.dynamic_slice_in_dim(
        residual[per_device * n_ep :], lax.axis_index("tp") * part_width, part_width, 1
    )
    return (own_residual + mixed).astype(bf16)


def solution(mesh):
    placed = (
        P("ep", None),
        P(),
        P("ep", "tp"),
        P(),
        P("ep", "tp", None, None),
        P("ep", "tp", None, None),
        P("ep"),
        P("tp", "ep"),
        P(),
        P("ep"),
        P("ep", None),
        P("ep", None),
        P("ep", None, "tp"),
        P("ep", None, "tp"),
        P("ep", "tp", None),
    )
    return jax.shard_map(body, mesh=mesh, in_specs=placed, out_specs=P("ep", "tp"), check_vma=False)
```

```python
import jax
import jax.numpy as jnp
from jax import lax
from jax.experimental import pallas as pl
from jax.experimental.pallas import tpu as pltpu
from jax.sharding import PartitionSpec as P

rms_epsilon = 1e-06
f32, bf16, i32 = jnp.float32, jnp.bfloat16, jnp.int32
in_vmem = pl.BlockSpec(memory_space=pltpu.VMEM)
in_smem = pl.BlockSpec(memory_space=pltpu.SMEM)


params = pltpu.CompilerParams(vmem_limit_bytes=24 * 1024 * 1024)


def near(array):
    return pltpu.with_memory_space_constraint(array, pltpu.VMEM)


def send_kernel(hidden_ref, group_ref, inner_ref, out_ref, *, group_size):
    n_ep, height, rows = out_ref.shape
    top_k, tokens = inner_ref.shape
    lane = lax.broadcasted_iota(i32, (tokens, rows), 1)
    ids = jnp.zeros((tokens, rows), f32)
    for t in range(tokens):
        for k in range(top_k):
            value = (group_ref[t] * group_size + inner_ref[k, t]).astype(f32)
            ids = jnp.where(lane == t * top_k + k, value, ids)
    for e in range(n_ep):
        part = hidden_ref[:, e * rows : (e + 1) * rows].astype(f32)
        out_ref[e] = jnp.concatenate([part, ids], axis=0).astype(bf16)


def query_kernel(features_ref, gain_ref, weight_ref, out_ref, *, tokens):
    n_ep, height, rows = features_ref.shape
    heads = out_ref.shape[1] // tokens
    size = out_ref.shape[2]
    start = pl.multiple_of(lax.axis_index("ep") * rows, 128)
    gain = gain_ref[:, pl.ds(start, rows)]
    flat = features_ref[...].astype(f32).reshape(n_ep * height, rows)
    parts = jnp.dot((flat * gain).astype(bf16), weight_ref[...], preferred_element_type=f32)
    parts = parts.reshape(n_ep, height, heads * size)
    for h in range(heads):
        out_ref[:, h * tokens : (h + 1) * tokens, :] = parts[:, :tokens, h * size : (h + 1) * size]


def attend_kernel(
    parts_ref, hidden_ref, keys_ref, values_ref, lengths_ref, bias_ref, out_ref, key_ref, value_ref, sems
):
    tokens, _, cache, size = key_ref.shape
    loads = [pltpu.make_async_copy(keys_ref.at[t], key_ref.at[t], sems.at[0, t]) for t in range(tokens)]
    loads += [pltpu.make_async_copy(values_ref.at[t], value_ref.at[t], sems.at[1, t]) for t in range(tokens)]
    for load in loads:
        load.start()
    n_ep, rows, _ = parts_ref.shape
    heads = rows // tokens
    chunk = 128
    wide = hidden_ref[...].astype(f32)
    scale = lax.rsqrt(jnp.mean(wide * wide, axis=-1, keepdims=True) + rms_epsilon)
    queries = jnp.sum(parts_ref[...], axis=0) * jnp.concatenate([scale] * heads, axis=0)
    queries = queries.astype(bf16)
    row = lax.broadcasted_iota(i32, (rows, 1), 0)
    token_of, head_of = row % tokens, row // tokens
    bias = jnp.zeros((rows, 1), f32)
    first = lax.axis_index("tp") * heads
    for h in range(heads):
        bias = jnp.where(head_of == h, bias_ref[first + h], bias)
    length = jnp.zeros((rows, 1), i32)
    for t in range(tokens):
        length = jnp.where(token_of == t, lengths_ref[t], length)
    scores = jnp.zeros((rows, cache), f32)
    for t in range(tokens):
        loads[t].wait()
        found = lax.dot_general(
            queries, key_ref[t, 0], (((1,), (1,)), ((), ())), preferred_element_type=f32
        )
        scores = jnp.where(token_of == t, found, scores)
    scores = scores * size ** (-0.5) + bias
    visible = lax.broadcasted_iota(i32, (rows, cache), 1) < length
    soft = jnp.log1p(jnp.exp(-jnp.abs(scores)))
    log_keep = jnp.where(visible, -jnp.maximum(scores, 0.0) - soft, 0.0)
    log_take = jnp.minimum(scores, 0.0) - soft
    count = cache // chunk
    stacked = jnp.concatenate([log_keep[:, c * chunk : (c + 1) * chunk] for c in range(count)], axis=0)
    later = (
        lax.broadcasted_iota(i32, (chunk, chunk), 0) > lax.broadcasted_iota(i32, (chunk, chunk), 1)
    ).astype(f32)
    inner = jnp.dot(stacked, later, preferred_element_type=f32, precision=lax.Precision.HIGHEST)
    totals = jnp.sum(stacked, axis=1, keepdims=True)
    running = jnp.zeros((rows, 1), f32)
    pieces = [None] * count
    for c in reversed(range(count)):
        pieces[c] = inner[c * rows : (c + 1) * rows] + running
        running = running + totals[c * rows : (c + 1) * rows]
    later_sum = jnp.concatenate(pieces, axis=1)
    weight = jnp.where(visible, jnp.exp(log_take + later_sum), 0.0).astype(bf16)
    result = jnp.zeros((rows, size), f32)
    for t in range(tokens):
        loads[tokens + t].wait()
        found = jnp.dot(weight, value_ref[t, 0], preferred_element_type=f32)
        result = jnp.where(token_of == t, found, result)
    result = result.astype(bf16)
    for e in range(n_ep):
        out_ref[e] = result


def pick_kernel(packed_ref, out_ref, *, tokens, top_k):
    n_ep, height, rows = packed_ref.shape
    shape = out_ref.shape
    message_rows = shape[0] // n_ep
    ids = packed_ref[...].astype(f32)[:, tokens, :]
    lane = lax.broadcasted_iota(i32, (rows, shape[1]), 0)
    column = lax.broadcasted_iota(i32, (rows, shape[1]), 1)
    owner = lax.broadcasted_iota(i32, (n_ep, shape[1]), 0)
    column_block = lax.broadcasted_iota(i32, (n_ep, shape[1]), 1) // height
    row = lax.broadcasted_iota(i32, shape, 0)
    expert, slot = row // message_rows, row % message_rows
    place = lax.broadcasted_iota(i32, shape, 1)
    block, place = place // height, place % height
    hit = jnp.zeros(shape, jnp.bool_)
    for k in range(top_k):
        spread = (lane == (column % height) * top_k + k).astype(f32)
        found = jnp.dot(ids, spread, preferred_element_type=f32, precision=lax.Precision.HIGHEST)
        found = jnp.sum(jnp.where(owner == column_block, found, 0.0), axis=0, keepdims=True)
        hit = hit | (found == expert.astype(f32))
    routed = (slot == block) & hit
    own = (block == expert) & (slot == n_ep + place)
    out_ref[...] = ((routed | own) & (place < tokens)).astype(f32).astype(bf16)


def project_kernel(heads_ref, weight_ref, features_ref, pick_ref, out_ref, *, tokens, n_tp):
    n_ep, rows, size = heads_ref.shape
    heads = rows // tokens
    height, columns = features_ref.shape[1:]
    flat = heads_ref[...].reshape(n_ep * rows, size)
    total = features_ref[...].astype(f32) * (1.0 / n_tp)
    total = total[:, :tokens, :]
    for h in range(heads):
        found = jnp.dot(
            flat, weight_ref[h * size : (h + 1) * size, :], preferred_element_type=f32
        ).reshape(n_ep, rows, columns)
        total = total + found[:, h * tokens : (h + 1) * tokens, :]
    total = jnp.concatenate([total, jnp.zeros((n_ep, height - tokens, columns), f32)], axis=1)
    total = total.reshape(n_ep * height, columns).astype(bf16)
    message = jnp.dot(pick_ref[...], total, preferred_element_type=f32).astype(bf16)
    message = message.reshape(n_ep, out_ref.shape[2], columns)
    for g in range(n_tp):
        out_ref[:, g] = message


def expert_kernel(parts_ref, gain_ref, gate_ref, up_ref, down_ref, out_ref, own_ref, *, tokens):
    n_ep, n_tp, height, columns = parts_ref.shape
    size = out_ref.shape[2]
    pieces = []
    for e in range(n_ep):
        piece = parts_ref[e, 0].astype(f32)
        for g in range(1, n_tp):
            piece = piece + parts_ref[e, g].astype(f32)
        pieces.append(piece)
    residual = jnp.concatenate(pieces, axis=1)
    own_ref[...] = residual[n_ep:, :]
    arrived = residual[:n_ep, :]
    arrived = arrived * lax.rsqrt(jnp.mean(arrived * arrived, axis=-1, keepdims=True) + rms_epsilon)
    arrived = (arrived * gain_ref[...]).astype(bf16)
    across = (((1,), (1,)), ((), ()))
    gated = lax.dot_general(arrived, gate_ref[0], across, preferred_element_type=f32)
    up = lax.dot_general(arrived, up_ref[0], across, preferred_element_type=f32)
    active = (gated / (1.0 + jnp.exp(-gated)) * up).astype(bf16)
    down = jnp.dot(active, down_ref[0], preferred_element_type=f32)
    for j in range(out_ref.shape[1]):
        out_ref[:, j, :] = down[:, j * size : (j + 1) * size]


def fast_body(
    hidden,
    attn_gain,
    query_weight,
    head_bias,
    key_cache,
    value_cache,
    lengths,
    out_weight,
    moe_gain,
    route_group,
    route_inner,
    route_weight,
    gate_w,
    up_w,
    down_w,
):
    n_tp = lax.axis_size("tp")
    n_ep = lax.axis_size("ep")
    tokens, d_model = hidden.shape
    rows, width = query_weight.shape
    columns = out_weight.shape[1]
    size = key_cache.shape[3]
    heads = width // size
    experts = n_ep
    group_size = experts // max(2, experts // 32)
    top_k = route_inner.shape[1]
    height = 2 * tokens
    part_width = d_model // n_tp
    call = pl.pallas_call

    packed = call(
        lambda *refs: send_kernel(*refs, group_size=group_size),
        name="send",
        out_shape=jax.ShapeDtypeStruct((n_ep, height, rows), bf16),
        in_specs=[in_vmem, in_smem, in_smem],
        out_specs=in_vmem,
        compiler_params=params,
    )(hidden, route_group, route_inner.T)
    packed = lax.all_to_all(packed, "ep", split_axis=0, concat_axis=0, tiled=True)

    parts = call(
        lambda *refs: query_kernel(*refs, tokens=tokens),
        name="query",
        out_shape=jax.ShapeDtypeStruct((n_ep, heads * tokens, size), f32),
        in_specs=[in_vmem] * 3,
        out_specs=in_vmem,
        compiler_params=params,
    )(near(packed), near(attn_gain.reshape(1, d_model)), near(query_weight))
    parts = lax.all_to_all(parts, "ep", split_axis=0, concat_axis=0, tiled=True)

    heads_out = call(
        attend_kernel,
        name="attend",
        out_shape=jax.ShapeDtypeStruct((n_ep, heads * tokens, size), bf16),
        in_specs=[in_vmem] * 2 + [pl.BlockSpec(memory_space=pl.ANY)] * 2 + [in_smem] * 2,
        out_specs=in_vmem,
        scratch_shapes=[
            pltpu.VMEM(key_cache.shape, key_cache.dtype),
            pltpu.VMEM(value_cache.shape, value_cache.dtype),
            pltpu.SemaphoreType.DMA((2, tokens)),
        ],
        compiler_params=params,
    )(near(parts), near(hidden), key_cache, value_cache, lengths, head_bias)
    heads_out = lax.all_to_all(heads_out, "ep", split_axis=0, concat_axis=0, tiled=True)

    message_rows = -(-(n_ep + tokens) // 16) * 16
    pick = call(
        lambda *refs: pick_kernel(*refs, tokens=tokens, top_k=top_k),
        name="pick",
        out_shape=jax.ShapeDtypeStruct((n_ep * message_rows, n_ep * height), bf16),
        in_specs=[in_vmem],
        out_specs=in_vmem,
        compiler_params=params,
    )(near(packed))

    message = call(
        lambda *refs: project_kernel(*refs, tokens=tokens, n_tp=n_tp),
        name="project",
        out_shape=jax.ShapeDtypeStruct((n_ep, n_tp, message_rows, columns), bf16),
        in_specs=[in_vmem] * 4,
        out_specs=in_vmem,
        compiler_params=params,
    )(near(heads_out), near(out_weight), near(packed), near(pick))
    message = message.reshape(n_ep * n_tp, message_rows, columns)
    message = lax.all_to_all(message, ("ep", "tp"), split_axis=0, concat_axis=0, tiled=True)

    down_out, own = call(
        lambda *refs: expert_kernel(*refs, tokens=tokens),
        name="expert",
        out_shape=(
            jax.ShapeDtypeStruct((n_ep, d_model // size, size), f32),
            jax.ShapeDtypeStruct((message_rows - n_ep, d_model), f32),
        ),
        in_specs=[in_vmem] * 5,
        out_specs=(in_vmem, in_vmem),
        compiler_params=params,
    )(
        near(message.reshape(n_ep, n_tp, message_rows, columns)),
        near(moe_gain.reshape(1, d_model)),
        near(gate_w.swapaxes(1, 2)),
        near(up_w.swapaxes(1, 2)),
        near(down_w),
    )
    lanes = part_width // size
    returned = lax.all_to_all(
        down_out.reshape(n_ep * n_tp, lanes, size), ("ep", "tp"), split_axis=0, concat_axis=0, tiled=True
    )
    returned = returned.reshape(n_ep, n_tp, lanes, size).sum(axis=1)
    chosen = route_group[:, None] * group_size + route_inner
    matches = chosen[:, :, None] == jnp.arange(experts, dtype=i32)[None, None, :]
    mixing = jnp.sum(jnp.where(matches, route_weight[:, :, None].astype(f32), 0.0), axis=1)
    mixed = jnp.sum(mixing[:, :, None, None] * returned[None], axis=1).reshape(tokens, part_width)
    own = lax.dynamic_slice_in_dim(own[:tokens], lax.axis_index("tp") * part_width, part_width, 1)
    return (own + mixed).astype(bf16)


def body(*args):
    hidden, query_weight, key_cache = args[0], args[2], args[4]
    out_weight, gate_w = args[7], args[12]
    aligned = all(
        extent % 128 == 0
        for extent in (query_weight.shape[0], query_weight.shape[1], out_weight.shape[1])
    )
    single = gate_w.shape[0] == 1 and key_cache.shape[1] == 1
    shapes = hidden.shape[0] == 4 and key_cache.shape[3] == 128 and key_cache.shape[2] % 128 == 0
    return fast_body(*args) if aligned and single and shapes else plain_body(*args)


def plain_body(
    hidden,
    attn_gain,
    query_weight,
    head_bias,
    key_cache,
    value_cache,
    lengths,
    out_weight,
    moe_gain,
    route_group,
    route_inner,
    route_weight,
    gate_w,
    up_w,
    down_w,
):
    f32, bf16 = jnp.float32, jnp.bfloat16
    n_tp = lax.axis_size("tp")
    n_ep = lax.axis_size("ep")
    tokens, d_model = hidden.shape
    rows = query_weight.shape[0]
    per_device = gate_w.shape[0]
    experts = per_device * n_ep
    group_count = max(2, experts // 32)
    group_size = experts // group_count
    top_k = route_inner.shape[1]
    chosen = route_group[:, None] * group_size + route_inner

    blocks = hidden.reshape(tokens, n_ep, rows).transpose(1, 0, 2).reshape(n_ep, tokens * rows)
    ids = jnp.broadcast_to(chosen.astype(bf16).reshape(1, tokens * top_k), (n_ep, tokens * top_k))
    ids = jnp.pad(ids, ((0, 0), (0, 128 - tokens * top_k)))
    packed = jnp.concatenate([blocks, ids], axis=1)
    packed = lax.all_to_all(packed, "ep", split_axis=0, concat_axis=0, tiled=True)
    all_tokens = n_ep * tokens
    features = packed[:, : tokens * rows].reshape(all_tokens, rows)
    all_chosen = packed[:, tokens * rows : tokens * (rows + top_k)].reshape(all_tokens, top_k)
    all_chosen = all_chosen.astype(jnp.int32)

    ep_index = lax.axis_index("ep")
    gain_block = lax.dynamic_slice_in_dim(attn_gain, ep_index * rows, rows, 0)
    scaled = (features.astype(f32) * gain_block).astype(bf16)
    parts = jnp.dot(scaled, query_weight, preferred_element_type=f32)
    width = parts.shape[1]

    parts = lax.all_to_all(
        parts.reshape(n_ep, tokens * width), "ep", split_axis=0, concat_axis=0, tiled=True
    )
    wide = hidden.astype(f32)
    row_scale = lax.rsqrt(jnp.mean(wide * wide, axis=-1, keepdims=True) + rms_epsilon)
    queries = parts.sum(axis=0).reshape(tokens, width) * row_scale
    queries = queries.astype(bf16)

    head_size = key_cache.shape[3]
    local_kv = key_cache.shape[1]
    cache_len = key_cache.shape[2]
    local_heads = width // head_size
    group_heads = local_heads // local_kv
    queries = queries.reshape(tokens, local_kv, group_heads, head_size)
    own_bias = lax.dynamic_slice_in_dim(
        head_bias, lax.axis_index("tp") * local_heads, local_heads, 0
    )
    own_bias = own_bias.reshape(local_kv, group_heads)
    scores = jnp.einsum(
        "tkgd,tkpd->tkgp", queries, key_cache, preferred_element_type=f32
    ) * head_size ** (-0.5)
    scores = scores + own_bias[None, :, :, None]
    position = jnp.arange(cache_len, dtype=jnp.int32)
    visible = position[None, None, None, :] < lengths[:, None, None, None]
    soft = jnp.log1p(jnp.exp(-jnp.abs(scores)))
    log_keep = jnp.where(visible, -jnp.maximum(scores, 0.0) - soft, 0.0)
    n_chunk = cache_len // 128
    chunked = log_keep.reshape(tokens, local_kv, group_heads, n_chunk, 128)
    lower = (jnp.arange(128)[:, None] > jnp.arange(128)[None, :]).astype(f32)
    inner = jnp.einsum("tkgcp,pq->tkgcq", chunked, lower, precision=lax.Precision.HIGHEST)
    totals = chunked.sum(axis=-1)
    later_chunks = jnp.arange(n_chunk)[:, None] > jnp.arange(n_chunk)[None, :]
    outer = jnp.where(later_chunks, totals[..., :, None], 0.0).sum(axis=-2)
    later_sum = (inner + outer[..., None]).reshape(scores.shape)
    weight = jnp.where(visible, jnp.exp(jnp.minimum(scores, 0.0) - soft + later_sum), 0.0)
    heads_out = jnp.einsum(
        "tkgp,tkpd->tkgd", weight.astype(bf16), value_cache, preferred_element_type=f32
    )
    heads_out = heads_out.astype(bf16).reshape(1, tokens * width)

    gathered = lax.all_to_all(
        jnp.broadcast_to(heads_out, (n_ep, tokens * width)), "ep", split_axis=0, concat_axis=0, tiled=True
    ).reshape(all_tokens, width)
    partial = jnp.dot(gathered, out_weight, preferred_element_type=f32)
    columns = out_weight.shape[1]
    partial = (partial + features.astype(f32) * (1.0 / n_tp)).astype(bf16)

    by_block = all_chosen.reshape(n_ep, tokens, top_k)
    hits = by_block[None] == jnp.arange(experts, dtype=jnp.int32)[:, None, None, None]
    hits = jnp.any(hits, axis=3).astype(bf16)
    routed = jnp.einsum(
        "ebt,btc->ebc", hits, partial.reshape(n_ep, tokens, columns), preferred_element_type=f32
    ).astype(bf16)
    routed = routed.reshape(n_ep, per_device * n_ep * columns)
    message = jnp.concatenate([routed, partial.reshape(n_ep, tokens * columns)], axis=1)
    length = message.shape[1]
    message = jnp.broadcast_to(message[:, None], (n_ep, n_tp, length)).reshape(n_ep * n_tp, length)
    received = lax.all_to_all(message, ("ep", "tp"), split_axis=0, concat_axis=0, tiled=True)
    received = received.reshape(n_ep, n_tp, per_device * n_ep + tokens, columns)
    summed = received.astype(f32).sum(axis=1)
    residual = summed.transpose(1, 0, 2).reshape(per_device * n_ep + tokens, d_model)
    arrived = residual[: per_device * n_ep]
    arrived = arrived * lax.rsqrt(jnp.mean(arrived * arrived, axis=-1, keepdims=True) + rms_epsilon)
    arrived = (arrived * moe_gain).astype(bf16).reshape(per_device, n_ep, d_model)
    gated_in = jnp.einsum("esd,edf->esf", arrived, gate_w, preferred_element_type=f32)
    up_proj = jnp.einsum("esd,edf->esf", arrived, up_w, preferred_element_type=f32)
    activated = (jax.nn.silu(gated_in) * up_proj).astype(bf16)
    down_out = jnp.einsum("esf,efd->sed", activated, down_w, preferred_element_type=f32).astype(bf16)

    part_width = d_model // n_tp
    down_out = down_out.reshape(n_ep, per_device, n_tp, part_width).transpose(0, 2, 1, 3)
    returned = lax.all_to_all(
        down_out.reshape(n_ep * n_tp, per_device * part_width), ("ep", "tp"), split_axis=0, concat_axis=0, tiled=True
    )
    returned = returned.reshape(n_ep, n_tp, per_device, part_width).astype(f32).sum(axis=1)
    returned = returned.reshape(experts, part_width)
    matches = chosen[:, :, None] == jnp.arange(experts, dtype=jnp.int32)[None, None, :]
    mixing = jnp.sum(jnp.where(matches, route_weight[:, :, None].astype(f32), 0.0), axis=1)
    mixed = jnp.sum(mixing[:, :, None] * returned[None], axis=1)
    own_residual = lax.dynamic_slice_in_dim(
        residual[per_device * n_ep :], lax.axis_index("tp") * part_width, part_width, 1
    )
    return (own_residual + mixed).astype(bf16)


def solution(mesh):
    placed = (
        P("ep", None),
        P(),
        P("ep", "tp"),
        P(),
        P("ep", "tp", None, None),
        P("ep", "tp", None, None),
        P("ep"),
        P("tp", "ep"),
        P(),
        P("ep"),
        P("ep", None),
        P("ep", None),
        P("ep", None, "tp"),
        P("ep", None, "tp"),
        P("ep", "tp", None),
    )
    return jax.shard_map(body, mesh=mesh, in_specs=placed, out_specs=P("ep", "tp"), check_vma=False)
```

```python
import jax
import jax.numpy as jnp
from jax import lax
from jax.experimental import pallas as pl
from jax.experimental.pallas import tpu as pltpu
from jax.sharding import PartitionSpec as P

rms_epsilon = 1e-06
f32, bf16, i32 = jnp.float32, jnp.bfloat16, jnp.int32
in_vmem = pl.BlockSpec(memory_space=pltpu.VMEM)
in_smem = pl.BlockSpec(memory_space=pltpu.SMEM)


params = pltpu.CompilerParams(vmem_limit_bytes=24 * 1024 * 1024)


def near(array):
    return pltpu.with_memory_space_constraint(array, pltpu.VMEM)


def send_kernel(hidden_ref, group_ref, inner_ref, out_ref, *, group_size):
    n_ep, height, rows = out_ref.shape
    top_k, tokens = inner_ref.shape
    lane = lax.broadcasted_iota(i32, (tokens, rows), 1)
    ids = jnp.zeros((tokens, rows), f32)
    for t in range(tokens):
        for k in range(top_k):
            value = (group_ref[t] * group_size + inner_ref[k, t]).astype(f32)
            ids = jnp.where(lane == t * top_k + k, value, ids)
    for e in range(n_ep):
        part = hidden_ref[:, e * rows : (e + 1) * rows].astype(f32)
        out_ref[e] = jnp.concatenate([part, ids], axis=0).astype(bf16)


def query_kernel(features_ref, gain_ref, weight_ref, out_ref, *, tokens):
    n_ep, height, rows = features_ref.shape
    heads = out_ref.shape[1] // tokens
    size = out_ref.shape[2]
    start = pl.multiple_of(lax.axis_index("ep") * rows, 128)
    gain = gain_ref[:, pl.ds(start, rows)]
    flat = features_ref[...].astype(f32).reshape(n_ep * height, rows)
    parts = jnp.dot((flat * gain).astype(bf16), weight_ref[...], preferred_element_type=f32)
    parts = parts.reshape(n_ep, height, heads * size)
    for h in range(heads):
        out_ref[:, h * tokens : (h + 1) * tokens, :] = parts[:, :tokens, h * size : (h + 1) * size]


def attend_kernel(
    parts_ref, hidden_ref, keys_ref, values_ref, lengths_ref, bias_ref, out_ref, key_ref, value_ref, sems
):
    tokens, _, cache, size = key_ref.shape
    loads = [pltpu.make_async_copy(keys_ref.at[t], key_ref.at[t], sems.at[0, t]) for t in range(tokens)]
    loads += [pltpu.make_async_copy(values_ref.at[t], value_ref.at[t], sems.at[1, t]) for t in range(tokens)]
    for load in loads:
        load.start()
    n_ep, rows, _ = parts_ref.shape
    heads = rows // tokens
    chunk = 128
    wide = hidden_ref[...].astype(f32)
    scale = lax.rsqrt(jnp.mean(wide * wide, axis=-1, keepdims=True) + rms_epsilon)
    queries = jnp.sum(parts_ref[...], axis=0) * jnp.concatenate([scale] * heads, axis=0)
    queries = queries.astype(bf16)
    row = lax.broadcasted_iota(i32, (rows, 1), 0)
    token_of, head_of = row % tokens, row // tokens
    bias = jnp.zeros((rows, 1), f32)
    first = lax.axis_index("tp") * heads
    for h in range(heads):
        bias = jnp.where(head_of == h, bias_ref[first + h], bias)
    length = jnp.zeros((rows, 1), i32)
    for t in range(tokens):
        length = jnp.where(token_of == t, lengths_ref[t], length)
    scores = jnp.zeros((rows, cache), f32)
    for t in range(tokens):
        loads[t].wait()
        found = lax.dot_general(
            queries, key_ref[t, 0], (((1,), (1,)), ((), ())), preferred_element_type=f32
        )
        scores = jnp.where(token_of == t, found, scores)
    scores = scores * size ** (-0.5) + bias
    visible = lax.broadcasted_iota(i32, (rows, cache), 1) < length
    soft = jnp.log1p(jnp.exp(-jnp.abs(scores)))
    log_keep = jnp.where(visible, -jnp.maximum(scores, 0.0) - soft, 0.0)
    log_take = jnp.minimum(scores, 0.0) - soft
    count = cache // chunk
    stacked = jnp.concatenate([log_keep[:, c * chunk : (c + 1) * chunk] for c in range(count)], axis=0)
    later = (
        lax.broadcasted_iota(i32, (chunk, chunk), 0) > lax.broadcasted_iota(i32, (chunk, chunk), 1)
    ).astype(f32)
    inner = jnp.dot(stacked, later, preferred_element_type=f32, precision=lax.Precision.HIGHEST)
    totals = jnp.sum(stacked, axis=1, keepdims=True)
    running = jnp.zeros((rows, 1), f32)
    pieces = [None] * count
    for c in reversed(range(count)):
        pieces[c] = inner[c * rows : (c + 1) * rows] + running
        running = running + totals[c * rows : (c + 1) * rows]
    later_sum = jnp.concatenate(pieces, axis=1)
    weight = jnp.where(visible, jnp.exp(log_take + later_sum), 0.0).astype(bf16)
    result = jnp.zeros((rows, size), f32)
    for t in range(tokens):
        loads[tokens + t].wait()
        found = jnp.dot(weight, value_ref[t, 0], preferred_element_type=f32)
        result = jnp.where(token_of == t, found, result)
    result = result.astype(bf16)
    for e in range(n_ep):
        out_ref[e] = result


def pick_kernel(packed_ref, out_ref, *, tokens, top_k):
    n_ep, height, rows = packed_ref.shape
    shape = out_ref.shape
    message_rows = shape[0] // n_ep
    ids = packed_ref[...].astype(f32)[:, tokens, :]
    lane = lax.broadcasted_iota(i32, (rows, shape[1]), 0)
    column = lax.broadcasted_iota(i32, (rows, shape[1]), 1)
    owner = lax.broadcasted_iota(i32, (n_ep, shape[1]), 0)
    column_block = lax.broadcasted_iota(i32, (n_ep, shape[1]), 1) // height
    row = lax.broadcasted_iota(i32, shape, 0)
    expert, slot = row // message_rows, row % message_rows
    place = lax.broadcasted_iota(i32, shape, 1)
    block, place = place // height, place % height
    hit = jnp.zeros(shape, jnp.bool_)
    for k in range(top_k):
        spread = (lane == (column % height) * top_k + k).astype(f32)
        found = jnp.dot(ids, spread, preferred_element_type=f32, precision=lax.Precision.HIGHEST)
        found = jnp.sum(jnp.where(owner == column_block, found, 0.0), axis=0, keepdims=True)
        hit = hit | (found == expert.astype(f32))
    routed = (slot == block) & hit
    own = (block == expert) & (slot == n_ep + place)
    out_ref[...] = ((routed | own) & (place < tokens)).astype(f32).astype(bf16)


def project_kernel(heads_ref, weight_ref, features_ref, pick_ref, out_ref, *, tokens, n_tp):
    n_ep, rows, size = heads_ref.shape
    heads = rows // tokens
    height, columns = features_ref.shape[1:]
    flat = heads_ref[...].reshape(n_ep * rows, size)
    total = features_ref[...].astype(f32) * (1.0 / n_tp)
    total = total[:, :tokens, :]
    for h in range(heads):
        found = jnp.dot(
            flat, weight_ref[h * size : (h + 1) * size, :], preferred_element_type=f32
        ).reshape(n_ep, rows, columns)
        total = total + found[:, h * tokens : (h + 1) * tokens, :]
    total = jnp.concatenate([total, jnp.zeros((n_ep, height - tokens, columns), f32)], axis=1)
    total = total.reshape(n_ep * height, columns).astype(bf16)
    message = jnp.dot(pick_ref[...], total, preferred_element_type=f32)
    message = message.reshape(n_ep, pick_ref.shape[0] // n_ep, columns)
    lanes = out_ref.shape[3]
    starts = range(0, columns, lanes)
    pieces = [message[:, :n_ep, c : c + lanes] for c in starts]
    pieces += [message[:, n_ep : n_ep + tokens, c : c + lanes] for c in starts]
    message = jnp.concatenate(pieces, axis=1).astype(bf16)
    for g in range(n_tp):
        out_ref[:, g] = message


def expert_kernel(parts_ref, gain_ref, gate_ref, up_ref, down_ref, out_ref, own_ref, *, tokens):
    n_ep, n_tp, height, _ = parts_ref.shape
    size = out_ref.shape[2]
    count = height // (n_ep + tokens)
    pieces, own = [], []
    for e in range(n_ep):
        piece = parts_ref[e, 0].astype(f32)
        for g in range(1, n_tp):
            piece = piece + parts_ref[e, g].astype(f32)
        pieces += [piece[c * n_ep : (c + 1) * n_ep] for c in range(count)]
        rest = piece[count * n_ep :]
        own += [rest[c * tokens : (c + 1) * tokens] for c in range(count)]
    own_ref[...] = jnp.concatenate(own, axis=1)
    arrived = jnp.concatenate(pieces, axis=1)
    arrived = arrived * lax.rsqrt(jnp.mean(arrived * arrived, axis=-1, keepdims=True) + rms_epsilon)
    arrived = (arrived * gain_ref[...]).astype(bf16)
    across = (((1,), (1,)), ((), ()))
    gated = lax.dot_general(arrived, gate_ref[0], across, preferred_element_type=f32)
    up = lax.dot_general(arrived, up_ref[0], across, preferred_element_type=f32)
    active = (gated / (1.0 + jnp.exp(-gated)) * up).astype(bf16)
    down = jnp.dot(active, down_ref[0], preferred_element_type=f32)
    for j in range(out_ref.shape[1]):
        out_ref[:, j, :] = down[:, j * size : (j + 1) * size]


def fast_body(
    hidden,
    attn_gain,
    query_weight,
    head_bias,
    key_cache,
    value_cache,
    lengths,
    out_weight,
    moe_gain,
    route_group,
    route_inner,
    route_weight,
    gate_w,
    up_w,
    down_w,
):
    n_tp = lax.axis_size("tp")
    n_ep = lax.axis_size("ep")
    tokens, d_model = hidden.shape
    rows, width = query_weight.shape
    columns = out_weight.shape[1]
    size = key_cache.shape[3]
    heads = width // size
    experts = n_ep
    group_size = experts // max(2, experts // 32)
    top_k = route_inner.shape[1]
    height = 2 * tokens
    part_width = d_model // n_tp
    call = pl.pallas_call

    packed = call(
        lambda *refs: send_kernel(*refs, group_size=group_size),
        name="send",
        out_shape=jax.ShapeDtypeStruct((n_ep, height, rows), bf16),
        in_specs=[in_vmem, in_smem, in_smem],
        out_specs=in_vmem,
        compiler_params=params,
    )(hidden, route_group, route_inner.T)
    packed = lax.all_to_all(packed, "ep", split_axis=0, concat_axis=0, tiled=True)

    parts = call(
        lambda *refs: query_kernel(*refs, tokens=tokens),
        name="query",
        out_shape=jax.ShapeDtypeStruct((n_ep, heads * tokens, size), f32),
        in_specs=[in_vmem] * 3,
        out_specs=in_vmem,
        compiler_params=params,
    )(near(packed), near(attn_gain.reshape(1, d_model)), near(query_weight))
    parts = lax.all_to_all(parts, "ep", split_axis=0, concat_axis=0, tiled=True)

    heads_out = call(
        attend_kernel,
        name="attend",
        out_shape=jax.ShapeDtypeStruct((n_ep, heads * tokens, size), bf16),
        in_specs=[in_vmem] * 2 + [pl.BlockSpec(memory_space=pltpu.HBM)] * 2 + [in_smem] * 2,
        out_specs=in_vmem,
        scratch_shapes=[
            pltpu.VMEM(key_cache.shape, key_cache.dtype),
            pltpu.VMEM(value_cache.shape, value_cache.dtype),
            pltpu.SemaphoreType.DMA((2, tokens)),
        ],
        compiler_params=params,
    )(near(parts), near(hidden), key_cache, value_cache, lengths, head_bias)
    heads_out = lax.all_to_all(heads_out, "ep", split_axis=0, concat_axis=0, tiled=True)

    message_rows = -(-(n_ep + tokens) // 16) * 16
    pick = call(
        lambda *refs: pick_kernel(*refs, tokens=tokens, top_k=top_k),
        name="pick",
        out_shape=jax.ShapeDtypeStruct((n_ep * message_rows, n_ep * height), bf16),
        in_specs=[in_vmem],
        out_specs=in_vmem,
        compiler_params=params,
    )(near(packed))

    sent_rows = (n_ep + tokens) * columns // size
    message = call(
        lambda *refs: project_kernel(*refs, tokens=tokens, n_tp=n_tp),
        name="project",
        out_shape=jax.ShapeDtypeStruct((n_ep, n_tp, sent_rows, size), bf16),
        in_specs=[in_vmem] * 4,
        out_specs=in_vmem,
        compiler_params=params,
    )(near(heads_out), near(out_weight), near(packed), near(pick))
    message = message.reshape(n_ep * n_tp, sent_rows, size)
    message = lax.all_to_all(message, ("ep", "tp"), split_axis=0, concat_axis=0, tiled=True)

    down_out, own = call(
        lambda *refs: expert_kernel(*refs, tokens=tokens),
        name="expert",
        out_shape=(
            jax.ShapeDtypeStruct((n_ep, d_model // size, size), f32),
            jax.ShapeDtypeStruct((tokens, d_model), f32),
        ),
        in_specs=[in_vmem] * 5,
        out_specs=(in_vmem, in_vmem),
        compiler_params=params,
    )(
        near(message.reshape(n_ep, n_tp, sent_rows, size)),
        near(moe_gain.reshape(1, d_model)),
        near(gate_w.swapaxes(1, 2)),
        near(up_w.swapaxes(1, 2)),
        near(down_w),
    )
    lanes = part_width // size
    returned = lax.all_to_all(
        down_out.reshape(n_ep * n_tp, lanes, size), ("ep", "tp"), split_axis=0, concat_axis=0, tiled=True
    )
    returned = returned.reshape(n_ep, n_tp, lanes, size).sum(axis=1)
    chosen = route_group[:, None] * group_size + route_inner
    matches = chosen[:, :, None] == jnp.arange(experts, dtype=i32)[None, None, :]
    mixing = jnp.sum(jnp.where(matches, route_weight[:, :, None].astype(f32), 0.0), axis=1)
    mixed = jnp.sum(mixing[:, :, None, None] * returned[None], axis=1).reshape(tokens, part_width)
    own = lax.dynamic_slice_in_dim(own, lax.axis_index("tp") * part_width, part_width, 1)
    return (own + mixed).astype(bf16)


def body(*args):
    hidden, query_weight, key_cache = args[0], args[2], args[4]
    out_weight, gate_w = args[7], args[12]
    aligned = all(
        extent % 128 == 0
        for extent in (query_weight.shape[0], query_weight.shape[1], out_weight.shape[1])
    )
    single = gate_w.shape[0] == 1 and key_cache.shape[1] == 1
    shapes = hidden.shape[0] == 4 and key_cache.shape[3] == 128 and key_cache.shape[2] % 128 == 0
    shapes = shapes and hidden.shape[1] // query_weight.shape[0] % 8 == 0
    return fast_body(*args) if aligned and single and shapes else plain_body(*args)


def plain_body(
    hidden,
    attn_gain,
    query_weight,
    head_bias,
    key_cache,
    value_cache,
    lengths,
    out_weight,
    moe_gain,
    route_group,
    route_inner,
    route_weight,
    gate_w,
    up_w,
    down_w,
):
    f32, bf16 = jnp.float32, jnp.bfloat16
    n_tp = lax.axis_size("tp")
    n_ep = lax.axis_size("ep")
    tokens, d_model = hidden.shape
    rows = query_weight.shape[0]
    per_device = gate_w.shape[0]
    experts = per_device * n_ep
    group_count = max(2, experts // 32)
    group_size = experts // group_count
    top_k = route_inner.shape[1]
    chosen = route_group[:, None] * group_size + route_inner

    blocks = hidden.reshape(tokens, n_ep, rows).transpose(1, 0, 2).reshape(n_ep, tokens * rows)
    ids = jnp.broadcast_to(chosen.astype(bf16).reshape(1, tokens * top_k), (n_ep, tokens * top_k))
    ids = jnp.pad(ids, ((0, 0), (0, 128 - tokens * top_k)))
    packed = jnp.concatenate([blocks, ids], axis=1)
    packed = lax.all_to_all(packed, "ep", split_axis=0, concat_axis=0, tiled=True)
    all_tokens = n_ep * tokens
    features = packed[:, : tokens * rows].reshape(all_tokens, rows)
    all_chosen = packed[:, tokens * rows : tokens * (rows + top_k)].reshape(all_tokens, top_k)
    all_chosen = all_chosen.astype(jnp.int32)

    ep_index = lax.axis_index("ep")
    gain_block = lax.dynamic_slice_in_dim(attn_gain, ep_index * rows, rows, 0)
    scaled = (features.astype(f32) * gain_block).astype(bf16)
    parts = jnp.dot(scaled, query_weight, preferred_element_type=f32)
    width = parts.shape[1]

    parts = lax.all_to_all(
        parts.reshape(n_ep, tokens * width), "ep", split_axis=0, concat_axis=0, tiled=True
    )
    wide = hidden.astype(f32)
    row_scale = lax.rsqrt(jnp.mean(wide * wide, axis=-1, keepdims=True) + rms_epsilon)
    queries = parts.sum(axis=0).reshape(tokens, width) * row_scale
    queries = queries.astype(bf16)

    head_size = key_cache.shape[3]
    local_kv = key_cache.shape[1]
    cache_len = key_cache.shape[2]
    local_heads = width // head_size
    group_heads = local_heads // local_kv
    queries = queries.reshape(tokens, local_kv, group_heads, head_size)
    own_bias = lax.dynamic_slice_in_dim(
        head_bias, lax.axis_index("tp") * local_heads, local_heads, 0
    )
    own_bias = own_bias.reshape(local_kv, group_heads)
    scores = jnp.einsum(
        "tkgd,tkpd->tkgp", queries, key_cache, preferred_element_type=f32
    ) * head_size ** (-0.5)
    scores = scores + own_bias[None, :, :, None]
    position = jnp.arange(cache_len, dtype=jnp.int32)
    visible = position[None, None, None, :] < lengths[:, None, None, None]
    soft = jnp.log1p(jnp.exp(-jnp.abs(scores)))
    log_keep = jnp.where(visible, -jnp.maximum(scores, 0.0) - soft, 0.0)
    n_chunk = cache_len // 128
    chunked = log_keep.reshape(tokens, local_kv, group_heads, n_chunk, 128)
    lower = (jnp.arange(128)[:, None] > jnp.arange(128)[None, :]).astype(f32)
    inner = jnp.einsum("tkgcp,pq->tkgcq", chunked, lower, precision=lax.Precision.HIGHEST)
    totals = chunked.sum(axis=-1)
    later_chunks = jnp.arange(n_chunk)[:, None] > jnp.arange(n_chunk)[None, :]
    outer = jnp.where(later_chunks, totals[..., :, None], 0.0).sum(axis=-2)
    later_sum = (inner + outer[..., None]).reshape(scores.shape)
    weight = jnp.where(visible, jnp.exp(jnp.minimum(scores, 0.0) - soft + later_sum), 0.0)
    heads_out = jnp.einsum(
        "tkgp,tkpd->tkgd", weight.astype(bf16), value_cache, preferred_element_type=f32
    )
    heads_out = heads_out.astype(bf16).reshape(1, tokens * width)

    gathered = lax.all_to_all(
        jnp.broadcast_to(heads_out, (n_ep, tokens * width)), "ep", split_axis=0, concat_axis=0, tiled=True
    ).reshape(all_tokens, width)
    partial = jnp.dot(gathered, out_weight, preferred_element_type=f32)
    columns = out_weight.shape[1]
    partial = (partial + features.astype(f32) * (1.0 / n_tp)).astype(bf16)

    by_block = all_chosen.reshape(n_ep, tokens, top_k)
    hits = by_block[None] == jnp.arange(experts, dtype=jnp.int32)[:, None, None, None]
    hits = jnp.any(hits, axis=3).astype(bf16)
    routed = jnp.einsum(
        "ebt,btc->ebc", hits, partial.reshape(n_ep, tokens, columns), preferred_element_type=f32
    ).astype(bf16)
    routed = routed.reshape(n_ep, per_device * n_ep * columns)
    message = jnp.concatenate([routed, partial.reshape(n_ep, tokens * columns)], axis=1)
    length = message.shape[1]
    message = jnp.broadcast_to(message[:, None], (n_ep, n_tp, length)).reshape(n_ep * n_tp, length)
    received = lax.all_to_all(message, ("ep", "tp"), split_axis=0, concat_axis=0, tiled=True)
    received = received.reshape(n_ep, n_tp, per_device * n_ep + tokens, columns)
    summed = received.astype(f32).sum(axis=1)
    residual = summed.transpose(1, 0, 2).reshape(per_device * n_ep + tokens, d_model)
    arrived = residual[: per_device * n_ep]
    arrived = arrived * lax.rsqrt(jnp.mean(arrived * arrived, axis=-1, keepdims=True) + rms_epsilon)
    arrived = (arrived * moe_gain).astype(bf16).reshape(per_device, n_ep, d_model)
    gated_in = jnp.einsum("esd,edf->esf", arrived, gate_w, preferred_element_type=f32)
    up_proj = jnp.einsum("esd,edf->esf", arrived, up_w, preferred_element_type=f32)
    activated = (jax.nn.silu(gated_in) * up_proj).astype(bf16)
    down_out = jnp.einsum("esf,efd->sed", activated, down_w, preferred_element_type=f32).astype(bf16)

    part_width = d_model // n_tp
    down_out = down_out.reshape(n_ep, per_device, n_tp, part_width).transpose(0, 2, 1, 3)
    returned = lax.all_to_all(
        down_out.reshape(n_ep * n_tp, per_device * part_width), ("ep", "tp"), split_axis=0, concat_axis=0, tiled=True
    )
    returned = returned.reshape(n_ep, n_tp, per_device, part_width).astype(f32).sum(axis=1)
    returned = returned.reshape(experts, part_width)
    matches = chosen[:, :, None] == jnp.arange(experts, dtype=jnp.int32)[None, None, :]
    mixing = jnp.sum(jnp.where(matches, route_weight[:, :, None].astype(f32), 0.0), axis=1)
    mixed = jnp.sum(mixing[:, :, None] * returned[None], axis=1)
    own_residual = lax.dynamic_slice_in_dim(
        residual[per_device * n_ep :], lax.axis_index("tp") * part_width, part_width, 1
    )
    return (own_residual + mixed).astype(bf16)


def solution(mesh):
    placed = (
        P("ep", None),
        P(),
        P("ep", "tp"),
        P(),
        P("ep", "tp", None, None),
        P("ep", "tp", None, None),
        P("ep"),
        P("tp", "ep"),
        P(),
        P("ep"),
        P("ep", None),
        P("ep", None),
        P("ep", None, "tp"),
        P("ep", None, "tp"),
        P("ep", "tp", None),
    )
    return jax.shard_map(body, mesh=mesh, in_specs=placed, out_specs=P("ep", "tp"), check_vma=False)
```
